32 devices in a mesh: grp: 2 (over y), fs: 4 (over z), tp: 4 (over x, core).
Axes of the slice: x: 2, y: 2, z: 4, core: 2. Of those that a mesh axis runs over, the one named last changes fastest.
Arguments:
- tokens: bfloat16 [8192, 2048], P(('grp', 'fs', 'tp')), parts along dimension 0, may hold values from -6 to 6
- norm_gains: float32 [4, 2048], replicated, may hold values from 0.1 to 1.9
- query_weight: bfloat16 [2048, 2048], P('fs', 'tp'), may hold values from -0.125 to 0.125
- key_weight: bfloat16 [2048, 2048], P('fs', 'tp'), may hold values from -0.125 to 0.125
- value_weight: bfloat16 [2048, 4096], P('fs', 'tp'), may hold values from -0.125 to 0.125
- swish_weight: bfloat16 [2048, 4096], P('fs', 'tp'), may hold values from -0.125 to 0.125
- mixer_output: bfloat16 [4096, 2048], P('tp', 'fs'), may hold values from -0.09375 to 0.09375
- gate_weight: bfloat16 [2048, 3072], P('fs', 'tp'), may hold values from -0.125 to 0.125
- up_weight: bfloat16 [2048, 3072], P('fs', 'tp'), may hold values from -0.125 to 0.125
- down_weight: bfloat16 [3072, 2048], P('tp', 'fs'), may hold values from -0.109375 to 0.109375
Outputs:
- layer_output: bfloat16 [8192, 2048], P(('grp', 'fs', 'tp')), parts along dimension 0
The draws below stay inside these ranges and needn't reach their ends.
There are 2 independent parts, one for each index of `grp`. The reference program is written for one: setup_inputs(seed, part) draws one part's arguments, and reference() takes and returns one part's arrays. A program takes and returns all parts, laid end to end along the dimension named above; an argument that names none is the same for every part. Nothing has to cross between parts.
All inputs are finite; a program needn't handle non-finite values.
Results may differ from the reference program's by a relative error of at most 0.02.
Values may be sent and summed in bfloat16 or wider, within the bound.
A program may use at most 128 MiB of HBM per device.

```python
import jax
import jax.numpy as jnp
from jax import lax

D = 2048
H = 8
QK = 256
VD = 512
FF = 3072
BLOCK = 128
SEQ = 1024
TOKENS = 4096
N_TP = 4


def levels(own_key, shape, pieces, low, top_value):
    level, own = 1.0, jax.random.fold_in(own_key, 6)
    for dim, parts in pieces:
        draws = jnp.exp(jax.random.uniform(jax.random.fold_in(own, dim), (parts,), jnp.float32, low / len(pieces), top_value / len(pieces)))
        level = level * jnp.repeat(draws, shape[dim] // parts).reshape([-1 if axis == dim else 1 for axis in range(len(shape))])
    return level


def noise(key, extent, deviation, most, split=(), kind=jnp.bfloat16):
    level = levels(key, extent, split, -0.22, 0.18) if split else 1.0
    array = jax.random.normal(key, extent, jnp.float32) * deviation * level
    return jnp.minimum(jnp.maximum(array, -most), most).astype(kind)


def setup_inputs(seed: int = 0, part: int = 0) -> dict:
    key_of = jax.random.split(jax.random.key(seed), 11)
    part_splits = jax.random.split(jax.random.fold_in(key_of[10], part), 11)
    tokens = noise(part_splits[0], (TOKENS, D), 1.0, 6.0, ((0, 16),))
    norm_gains = jnp.clip(1.0 + 0.18 * jax.random.normal(key_of[1], (4, D), jnp.float32), 0.1, 1.9)
    query_weight = noise(key_of[2], (D, H * QK), D ** -0.5, 0.125, ((0, 4), (1, 4)))
    key_weight = noise(key_of[3], (D, H * QK), D ** -0.5, 0.125, ((0, 4), (1, 4)))
    value_weight = noise(key_of[4], (D, H * VD), D ** -0.5, 0.125, ((0, 4), (1, 4)))
    swish_weight = noise(key_of[5], (D, H * VD), D ** -0.5, 0.125, ((0, 4), (1, 4)))
    mixer_output = noise(key_of[6], (H * VD, D), (H * VD) ** -0.5, 0.09375, ((0, 4), (1, 4)))
    gate_weight = noise(key_of[7], (D, FF), D ** -0.5, 0.125, ((0, 4), (1, 4)))
    up_weight = noise(key_of[8], (D, FF), D ** -0.5, 0.125, ((0, 4), (1, 4)))
    down_weight = noise(key_of[9], (FF, D), FF ** -0.5, 0.109375, ((0, 4), (1, 4)))
    return dict(tokens=tokens, norm_gains=norm_gains, query_weight=query_weight, key_weight=key_weight, value_weight=value_weight, swish_weight=swish_weight, mixer_output=mixer_output, gate_weight=gate_weight, up_weight=up_weight, down_weight=down_weight)


norm_epsilon = 1e-06
group_epsilon = 0.01

def rms_scale(matrix, gain):
    return matrix * lax.rsqrt(lax.optimization_barrier(jnp.mean(matrix * matrix, axis=-1, keepdims=True)) + norm_epsilon) * gain

def rotate_halves(head_tensors, cosine_table, sine_table):
    half_width = head_tensors.shape[-1] // 2
    lower_half = head_tensors[..., :half_width]
    upper_half = head_tensors[..., half_width:]
    return jnp.concatenate([lower_half * cosine_table - upper_half * sine_table, lower_half * sine_table + upper_half * cosine_table], axis=-1)

def decayed_sum(queries, key_rows, value_rows, log_decay):
    query_expanded = queries.astype(jnp.float32)
    key_expanded = key_rows.astype(jnp.float32)
    value_wide = value_rows.astype(jnp.float32)
    retention_scores = jnp.einsum('fzy,czy->zfc', query_expanded, key_expanded)
    offsets = jnp.arange(queries.shape[0], dtype=jnp.float32)
    distance = offsets[:, None] - offsets[None, :]
    weights = jnp.where(distance >= 0, jnp.exp(log_decay[:, None, None] * jnp.maximum(distance, 0.0)), 0.0)
    return jnp.einsum('hnm,mhe->nhe', retention_scores * weights, value_wide)

def grouped_product(active, weight):
    group_width = active.shape[1] // N_TP
    running = jnp.zeros((active.shape[0], weight.shape[1]), jnp.float32)
    for group_index in range(N_TP):
        lower = group_index * group_width
        product = jnp.dot(active[:, lower:lower + group_width], weight[lower:lower + group_width], preferred_element_type=jnp.float32)
        rounded = lax.optimization_barrier(product.astype(jnp.bfloat16))
        running = running + rounded.astype(jnp.float32)
    return running

def reference(tokens, norm_gains, query_weight, key_weight, value_weight, swish_weight, mixer_output, gate_weight, up_weight, down_weight):
    residual = tokens.astype(jnp.float32)
    normed = rms_scale(residual, norm_gains[0]).astype(jnp.bfloat16)
    raw_query = jnp.dot(normed, query_weight, preferred_element_type=jnp.float32)
    raw_keys = jnp.dot(normed, key_weight, preferred_element_type=jnp.float32)
    raw_values = jnp.dot(normed, value_weight, preferred_element_type=jnp.float32)
    raw_swish = jnp.dot(normed, swish_weight, preferred_element_type=jnp.float32)
    seq_count = tokens.shape[0] // SEQ
    positions = jnp.arange(SEQ, dtype=jnp.float32)
    frequency = 10000.0 ** (-jnp.linspace(0.0, 1.0, QK // 2, dtype=jnp.float32))
    angles = positions[:, None] * frequency[None, :]
    cosine_table = jnp.cos(angles)[:, None, :]
    sine_table = jnp.sin(angles)[:, None, :]
    queries = rotate_halves(raw_query.reshape(seq_count, SEQ, H, QK), cosine_table, sine_table).astype(jnp.bfloat16)
    key_rows = (rotate_halves(raw_keys.reshape(seq_count, SEQ, H, QK), cosine_table, sine_table) * QK ** (-0.5)).astype(jnp.bfloat16)
    value_rows = raw_values.reshape(seq_count, SEQ, H, VD).astype(jnp.bfloat16)
    head_index = jnp.arange(H, dtype=jnp.float32)
    log_decay = -(4.0 / BLOCK) * (BLOCK / (32.0 * SEQ)) ** (head_index / (H - 1))
    retained = lax.map(lambda triple: decayed_sum(triple[0], triple[1], triple[2], log_decay), (queries, key_rows, value_rows))
    centred = retained - lax.optimization_barrier(jnp.mean(retained, axis=-1, keepdims=True))
    normalized = centred * lax.rsqrt(lax.optimization_barrier(jnp.mean(centred * centred, axis=-1, keepdims=True)) + group_epsilon)
    gated_rows = (jax.nn.silu(raw_swish) * normalized.reshape(tokens.shape[0], H * VD)).astype(jnp.bfloat16)
    mixer_total = grouped_product(gated_rows, mixer_output)
    after_mixer = residual + rms_scale(mixer_total, norm_gains[1])
    widened = rms_scale(after_mixer, norm_gains[2]).astype(jnp.bfloat16)
    gate_sum = jnp.dot(widened, gate_weight, preferred_element_type=jnp.float32)
    up_sum = jnp.dot(widened, up_weight, preferred_element_type=jnp.float32)
    hidden = (jax.nn.silu(gate_sum) * up_sum).astype(jnp.bfloat16)
    channel = grouped_product(hidden, down_weight)
    return (after_mixer + rms_scale(channel, norm_gains[3])).astype(jnp.bfloat16)
```

```python
import jax
import jax.numpy as jnp
from jax import lax
from jax.sharding import PartitionSpec as P

H = 8
QK = 256
BLOCK = 128


norm_epsilon = 1e-06
group_epsilon = 0.01


def rms_scale(matrix, gain):
    return (
        matrix * lax.rsqrt(jnp.mean(matrix * matrix, axis=-1, keepdims=True) + norm_epsilon) * gain
    )


def roll_blocks(array, shift, count, axis):
    size = array.shape[axis] // count
    twice = jnp.concatenate([array, array], axis=axis)
    return lax.dynamic_slice_in_dim(twice, shift * size, size * count, axis)


def from_ahead(array, axis_name, distance):
    count = lax.axis_size(axis_name)
    return lax.ppermute(
        array, axis_name, [((i + distance) % count, i) for i in range(count)]
    )


def gather_relative(shard, axis):
    copies = lax.axis_size("grp")
    turned = roll_blocks(shard, lax.axis_index("grp"), copies, axis)
    own = lax.slice_in_dim(turned, 0, shard.shape[axis] // copies, axis=axis)
    pieces = [turned]
    for distance in range(1, lax.axis_size("fs")):
        piece = from_ahead(own, "fs", distance)
        pieces.append(piece)
        for step in range(1, copies):
            pieces.append(from_ahead(piece, "grp", step))
    return pieces


def columns_to_relative(rows):
    fs, copies = lax.axis_size("fs"), lax.axis_size("grp")
    rows = roll_blocks(rows, lax.axis_index("fs"), fs, 1)
    parts = jnp.split(rows, fs, axis=1)
    return jnp.concatenate(
        [roll_blocks(part, lax.axis_index("grp"), copies, 1) for part in parts], axis=1
    )


def columns_from_relative(rows):
    fs, copies = lax.axis_size("fs"), lax.axis_size("grp")
    back = (copies - lax.axis_index("grp")) % copies
    parts = jnp.split(rows, fs, axis=1)
    rows = jnp.concatenate([roll_blocks(part, back, copies, 1) for part in parts], axis=1)
    return roll_blocks(rows, (fs - lax.axis_index("fs")) % fs, fs, 1)


def matmul(left, right):
    return jnp.dot(left, right, preferred_element_type=jnp.float32)


def take_columns(pieces, start, width):
    return jnp.concatenate([piece[:, start : start + width] for piece in pieces], axis=0)


def project_out(active, pieces):
    partial = matmul(active, jnp.concatenate(pieces, axis=1)).astype(jnp.bfloat16)
    total = lax.psum_scatter(partial, "tp", scatter_dimension=0, tiled=True)
    return columns_from_relative(total).astype(jnp.float32)


def rotate_halves(head, cosine_table, sine_table):
    half_width = head.shape[-1] // 2
    lower_half = head[:, :half_width]
    upper_half = head[:, half_width:]
    return jnp.concatenate(
        [
            lower_half * cosine_table - upper_half * sine_table,
            lower_half * sine_table + upper_half * cosine_table,
        ],
        axis=-1,
    )


def per_device(
    tokens,
    norm_gains,
    query_weight,
    key_weight,
    value_weight,
    swish_weight,
    mixer_output,
    gate_weight,
    up_weight,
    down_weight,
):
    projections = gather_relative(
        jnp.concatenate([query_weight, key_weight, value_weight, swish_weight], axis=1), 0
    )
    mixer_pieces = gather_relative(mixer_output, 1)
    widening = gather_relative(jnp.concatenate([gate_weight, up_weight], axis=1), 0)
    down_pieces = gather_relative(down_weight, 1)

    residual = tokens.astype(jnp.float32)
    normed = columns_to_relative(rms_scale(residual, norm_gains[0]).astype(jnp.bfloat16))
    normed = lax.all_gather(normed, "tp", axis=0, tiled=True)

    length = normed.shape[0]
    qk_width, v_width = query_weight.shape[1], value_weight.shape[1]
    head_count = qk_width // QK
    head_value = v_width // head_count
    positions = jnp.arange(length, dtype=jnp.float32)
    frequency = 10000.0 ** (-jnp.linspace(0.0, 1.0, QK // 2, dtype=jnp.float32))
    angles = positions[:, None] * frequency[None, :]
    cosine_table = jnp.cos(angles)
    sine_table = jnp.sin(angles)
    raw_query = matmul(normed, take_columns(projections, 0, qk_width))
    raw_keys = matmul(normed, take_columns(projections, qk_width, qk_width))
    values = matmul(normed, take_columns(projections, 2 * qk_width, v_width)).astype(jnp.bfloat16)
    raw_swish = matmul(normed, take_columns(projections, 2 * qk_width + v_width, v_width))

    distance = positions[:, None] - positions[None, :]
    gated = []
    for head in range(head_count):
        head_index = (lax.axis_index("tp") * head_count + head).astype(jnp.float32)
        log_decay = -(4.0 / BLOCK) * (BLOCK / (32.0 * length)) ** (head_index / (H - 1))
        columns = slice(head * QK, (head + 1) * QK)
        queries = rotate_halves(raw_query[:, columns], cosine_table, sine_table)
        keys = rotate_halves(raw_keys[:, columns], cosine_table, sine_table) * QK ** (-0.5)
        scores = lax.dot_general(
            queries.astype(jnp.bfloat16),
            keys.astype(jnp.bfloat16),
            (((1,), (1,)), ((), ())),
            preferred_element_type=jnp.float32,
        )
        weights = jnp.where(
            distance >= 0, jnp.exp(log_decay * jnp.maximum(distance, 0.0)), 0.0
        )
        columns = slice(head * head_value, (head + 1) * head_value)
        retained = matmul((scores * weights).astype(jnp.bfloat16), values[:, columns])
        centred = retained - jnp.mean(retained, axis=-1, keepdims=True)
        normalized = centred * lax.rsqrt(
            jnp.mean(centred * centred, axis=-1, keepdims=True) + group_epsilon
        )
        gated.append((jax.nn.silu(raw_swish[:, columns]) * normalized).astype(jnp.bfloat16))
    gated_rows = jnp.concatenate(gated, axis=1)
    mixer_total = project_out(gated_rows, mixer_pieces)
    after_mixer = residual + rms_scale(mixer_total, norm_gains[1])
    widened = columns_to_relative(rms_scale(after_mixer, norm_gains[2]).astype(jnp.bfloat16))
    widened = lax.all_gather(widened, "tp", axis=0, tiled=True)
    hidden_width = gate_weight.shape[1]
    gate_sum = matmul(widened, take_columns(widening, 0, hidden_width))
    up_sum = matmul(widened, take_columns(widening, hidden_width, hidden_width))
    hidden = (jax.nn.silu(gate_sum) * up_sum).astype(jnp.bfloat16)
    channel = project_out(hidden, down_pieces)
    return (after_mixer + rms_scale(channel, norm_gains[3])).astype(jnp.bfloat16)


def solution(mesh):
    placed = (
        P(("grp", "fs", "tp"), None),
        P(),
        P("fs", "tp"),
        P("fs", "tp"),
        P("fs", "tp"),
        P("fs", "tp"),
        P("tp", "fs"),
        P("fs", "tp"),
        P("fs", "tp"),
        P("tp", "fs"),
    )
    return jax.shard_map(
        per_device,
        mesh=mesh,
        in_specs=placed,
        out_specs=P(("grp", "fs", "tp"), None),
        check_vma=False,
    )
```

```python
import jax
import jax.numpy as jnp
from jax import lax
from jax.sharding import PartitionSpec as P

H = 8
QK = 256
BLOCK = 128


norm_epsilon = 1e-06
group_epsilon = 0.01


def rms_scale(matrix, gain):
    return (
        matrix * lax.rsqrt(jnp.mean(matrix * matrix, axis=-1, keepdims=True) + norm_epsilon) * gain
    )


def roll_blocks(array, shift, count, axis):
    size = array.shape[axis] // count
    twice = jnp.concatenate([array, array], axis=axis)
    return lax.dynamic_slice_in_dim(twice, shift * size, size * count, axis)


def gather_relative(shard, axis):
    copies = lax.axis_size("grp")
    size = shard.shape[axis] // copies
    own = lax.dynamic_slice_in_dim(shard, lax.axis_index("grp") * size, size, axis)
    held = lax.all_gather(own, "fs", axis=axis, tiled=True)
    pieces = [held]
    for step in range(1, copies):
        pieces.append(
            lax.ppermute(held, "grp", [((i + step) % copies, i) for i in range(copies)])
        )
    return pieces


def columns_to_relative(rows):
    fs, copies = lax.axis_size("fs"), lax.axis_size("grp")
    count, width = rows.shape
    blocks = rows.reshape(count, fs, copies, -1).transpose(0, 2, 1, 3)
    return roll_blocks(blocks.reshape(count, width), lax.axis_index("grp"), copies, 1)


def columns_from_relative(rows):
    fs, copies = lax.axis_size("fs"), lax.axis_size("grp")
    count, width = rows.shape
    rows = roll_blocks(rows, (copies - lax.axis_index("grp")) % copies, copies, 1)
    return rows.reshape(count, copies, fs, -1).transpose(0, 2, 1, 3).reshape(count, width)


def matmul(left, right):
    return jnp.dot(left, right, preferred_element_type=jnp.float32)


def project_in(rows, pieces):
    return matmul(rows, jnp.concatenate(pieces, axis=0))


def project_out(active, pieces):
    partial = matmul(active, jnp.concatenate(pieces, axis=1)).astype(jnp.bfloat16)
    total = lax.psum_scatter(partial, "tp", scatter_dimension=0, tiled=True)
    return columns_from_relative(total).astype(jnp.float32)


def rotate_halves(head, cosine_table, sine_table):
    half_width = head.shape[-1] // 2
    lower_half = head[:, :half_width]
    upper_half = head[:, half_width:]
    return jnp.concatenate(
        [
            lower_half * cosine_table - upper_half * sine_table,
            lower_half * sine_table + upper_half * cosine_table,
        ],
        axis=-1,
    )


def per_device(
    tokens,
    norm_gains,
    query_weight,
    key_weight,
    value_weight,
    swish_weight,
    mixer_output,
    gate_weight,
    up_weight,
    down_weight,
):
    residual = tokens.astype(jnp.float32)
    normed = columns_to_relative(rms_scale(residual, norm_gains[0]).astype(jnp.bfloat16))
    normed = lax.all_gather(normed, "tp", axis=0, tiled=True)

    length = normed.shape[0]
    qk_width, v_width = query_weight.shape[1], value_weight.shape[1]
    head_count = qk_width // QK
    head_value = v_width // head_count
    positions = jnp.arange(length, dtype=jnp.float32)
    frequency = 10000.0 ** (-jnp.linspace(0.0, 1.0, QK // 2, dtype=jnp.float32))
    angles = positions[:, None] * frequency[None, :]
    cosine_table = jnp.cos(angles)
    sine_table = jnp.sin(angles)
    raw_query = project_in(normed, gather_relative(query_weight, 0))
    raw_keys = project_in(normed, gather_relative(key_weight, 0))
    values = project_in(normed, gather_relative(value_weight, 0)).astype(jnp.bfloat16)
    raw_swish = project_in(normed, gather_relative(swish_weight, 0))
    mixer_pieces = gather_relative(mixer_output, 1)
    gate_pieces = gather_relative(gate_weight, 0)
    up_pieces = gather_relative(up_weight, 0)
    down_pieces = gather_relative(down_weight, 1)

    distance = positions[:, None] - positions[None, :]
    gated = []
    for head in range(head_count):
        head_index = (lax.axis_index("tp") * head_count + head).astype(jnp.float32)
        log_decay = -(4.0 / BLOCK) * (BLOCK / (32.0 * length)) ** (head_index / (H - 1))
        columns = slice(head * QK, (head + 1) * QK)
        queries = rotate_halves(raw_query[:, columns], cosine_table, sine_table)
        keys = rotate_halves(raw_keys[:, columns], cosine_table, sine_table) * QK ** (-0.5)
        scores = lax.dot_general(
            queries.astype(jnp.bfloat16),
            keys.astype(jnp.bfloat16),
            (((1,), (1,)), ((), ())),
            preferred_element_type=jnp.float32,
        )
        weights = jnp.where(
            distance >= 0, jnp.exp(log_decay * jnp.maximum(distance, 0.0)), 0.0
        )
        columns = slice(head * head_value, (head + 1) * head_value)
        retained = matmul((scores * weights).astype(jnp.bfloat16), values[:, columns])
        centred = retained - jnp.mean(retained, axis=-1, keepdims=True)
        normalized = centred * lax.rsqrt(
            jnp.mean(centred * centred, axis=-1, keepdims=True) + group_epsilon
        )
        gated.append((jax.nn.silu(raw_swish[:, columns]) * normalized).astype(jnp.bfloat16))
    gated_rows = jnp.concatenate(gated, axis=1)
    mixer_total = project_out(gated_rows, mixer_pieces)
    after_mixer = residual + rms_scale(mixer_total, norm_gains[1])
    widened = columns_to_relative(rms_scale(after_mixer, norm_gains[2]).astype(jnp.bfloat16))
    widened = lax.all_gather(widened, "tp", axis=0, tiled=True)
    gate_sum = project_in(widened, gate_pieces)
    up_sum = project_in(widened, up_pieces)
    hidden = (jax.nn.silu(gate_sum) * up_sum).astype(jnp.bfloat16)
    channel = project_out(hidden, down_pieces)
    return (after_mixer + rms_scale(channel, norm_gains[3])).astype(jnp.bfloat16)


def solution(mesh):
    placed = (
        P(("grp", "fs", "tp"), None),
        P(),
        P("fs", "tp"),
        P("fs", "tp"),
        P("fs", "tp"),
        P("fs", "tp"),
        P("tp", "fs"),
        P("fs", "tp"),
        P("fs", "tp"),
        P("tp", "fs"),
    )
    return jax.shard_map(
        per_device,
        mesh=mesh,
        in_specs=placed,
        out_specs=P(("grp", "fs", "tp"), None),
        check_vma=False,
    )
```
